32 devices in a mesh: sp: 8 (over z, x), tp: 4 (over y, core).
Axes of the slice: x: 2, y: 2, z: 4, core: 2. Of those that a mesh axis runs over, the one named last changes fastest.
Arguments:
- inputs: bfloat16 [8192, 2048], P('sp'), may hold values from -6 to 6
- w_query: bfloat16 [2048, 2048], P(None, 'tp'), may hold values from -0.125 to 0.125
- w_key: bfloat16 [2048, 2048], P(None, 'tp'), may hold values from -0.125 to 0.125
- w_value: bfloat16 [2048, 2048], P(None, 'tp'), may hold values from -0.125 to 0.125
- rel_table: float32 [16, 257], P('tp'), may hold values from -4 to 254
- out_grad: bfloat16 [8192, 2048], P('sp', 'tp'), may hold values from -6 to 6
Outputs:
- query_grad: bfloat16 [8192, 2048], P('sp', 'tp')
- key_grad: bfloat16 [8192, 2048], P('sp', 'tp')
- value_grad: bfloat16 [8192, 2048], P('sp', 'tp')
- query_weight_grad: float32 [2048, 2048], P('sp', 'tp')
- key_weight_grad: float32 [2048, 2048], P('sp', 'tp')
- value_weight_grad: float32 [2048, 2048], P('sp', 'tp')
- table_grad: float32 [16, 257], P('tp')
The draws below stay inside these ranges and needn't reach their ends.
All inputs are finite; a program needn't handle non-finite values.
Results may differ from the reference program's by a relative error of at most 0.017.
The reference program's roundings to bfloat16 on the way count: a program that leaves them out, or rounds other values in their place, can miss the bound.
Values may be sent and summed in bfloat16 or wider, within the bound.
A program may use at most 128 MiB of HBM per device.

```python
import jax
import jax.numpy as jnp
from jax import lax

HEADS = 16
HDIM = 128
D = 2048
SEG = 64
PREV = 4
MAXREL = 128
TOKENS = 8192


def draw_rel_table(key, part):
    base_key = jax.random.fold_in(jax.random.fold_in(key, 7), 0)
    bias_table = jnp.clip(jax.random.normal(base_key, (HEADS, 2 * MAXREL + 1), jnp.float32), -4.0, 4.0)
    return bias_table


def strengthened(drawn, own_key, source, target, parts, factor):
    owner, partner = [(jnp.arange(drawn.shape[axis_at]) // (drawn.shape[axis_at] // parts)).reshape([-1 if axis == axis_at else 1 for axis in range(drawn.ndim)]) for axis_at in (source, target)]
    chosen = jax.random.permutation(own_key, parts)[partner]
    strong = (owner == chosen) | (owner == (partner + parts // 2) % parts)
    return jnp.where(strong, factor * drawn, drawn)


def block_scale(rng, extent, pieces, least, high):
    factor_of = 1.0
    for dim, parts in pieces:
        steps = jax.random.uniform(jax.random.fold_in(jax.random.fold_in(rng, 6), dim), (parts,), jnp.float32, least / len(pieces), high / len(pieces))
        factor_of = factor_of * jnp.repeat(jnp.exp(steps), extent[dim] // parts).reshape((-1,) + (1,) * (len(extent) - 1 - dim))
    return factor_of


def normal_values(key, shape, spread, most, cuts=(), kind=jnp.bfloat16):
    values = spread * jax.random.normal(key, shape, jnp.float32)
    if cuts:
        values = values * block_scale(key, shape, cuts, -0.22, 0.18)
    return jnp.clip(values, -most, most).astype(kind)


def bell_draw_with(rng, shape, spread, bound, shards, heavy, held_as=jnp.bfloat16):
    array = spread * jax.random.normal(rng, shape, jnp.float32)
    if shards:
        array = array * block_scale(rng, shape, shards, -0.22, 0.18)
    return jnp.clip(strengthened(array, jax.random.fold_in(rng, 3), *heavy), -bound, bound).astype(held_as)


def setup_inputs(seed: int = 0) -> dict:
    streams_of = jax.random.split(jax.random.key(seed), 7)
    return {
        "inputs": bell_draw_with(streams_of[0], (TOKENS, D), 1.0, 6.0, ((0, 8),), (0, 1, 8, 2.0)),
        "w_query": normal_values(streams_of[1], (D, D), D ** -0.5, 0.125, ((1, 4),)),
        "w_key": normal_values(streams_of[2], (D, D), D ** -0.5, 0.125, ((1, 4),)),
        "w_value": normal_values(streams_of[3], (D, D), D ** -0.5, 0.125, ((1, 4),)),
        "rel_table": draw_rel_table(jax.random.fold_in(streams_of[6], 71), 0),
        "out_grad": normal_values(streams_of[5], (TOKENS, D), 1.0, 6.0, ((0, 8), (1, 4))),
    }


def project(inputs, weight):
    return jnp.dot(inputs, weight, preferred_element_type=jnp.float32).astype(jnp.bfloat16)


def reference(inputs, w_query, w_key, w_value, rel_table, out_grad):
    reach = PREV * SEG
    band = reach + SEG
    score_scale = HDIM ** -0.5
    query = project(inputs, w_query).reshape(TOKENS, HEADS, HDIM)
    key_rows = project(inputs, w_key).reshape(TOKENS, HEADS, HDIM)
    value_rows = project(inputs, w_value).reshape(TOKENS, HEADS, HDIM)
    upstream = out_grad.reshape(TOKENS, HEADS, HDIM)
    key_pad = jnp.pad(key_rows, ((reach, 0), (0, 0), (0, 0)))
    value_pad = jnp.pad(value_rows, ((reach, 0), (0, 0), (0, 0)))
    row_index = jnp.arange(SEG, dtype=jnp.int32)[:, None]
    band_index = jnp.arange(band, dtype=jnp.int32)[None, :]
    buckets = jnp.clip(row_index + reach - band_index, -MAXREL, MAXREL) + MAXREL
    bias_pattern = rel_table[:, buckets].astype(jnp.float32)

    def one_segment(carry, segment):
        key_acc, value_acc, pattern = carry
        start = segment * SEG
        query_seg = lax.dynamic_slice_in_dim(query, start, SEG, 0).astype(jnp.float32)
        grad_seg = lax.dynamic_slice_in_dim(upstream, start, SEG, 0).astype(jnp.float32)
        key_band = lax.dynamic_slice_in_dim(key_pad, start, band, 0).astype(jnp.float32)
        value_band = lax.dynamic_slice_in_dim(value_pad, start, band, 0).astype(jnp.float32)
        visible = band_index[0] >= reach - start
        scores = jnp.einsum('qhd,khd->hqk', query_seg, key_band) * score_scale + bias_pattern
        scores = jnp.where(visible[None, None, :], scores, -jnp.inf)
        row_max = jnp.max(scores, axis=-1, keepdims=True)
        log_norm = row_max + jnp.log(jnp.sum(jnp.exp(scores - row_max), axis=-1, keepdims=True))
        probs_full = jnp.exp(scores - log_norm)
        probs_low = lax.optimization_barrier(probs_full.astype(jnp.bfloat16)).astype(jnp.float32)
        attn_out = jnp.einsum('hqk,khd->qhd', probs_low, value_band)
        attn_out = lax.optimization_barrier(attn_out.astype(jnp.bfloat16)).astype(jnp.float32)
        out_dot = jnp.sum(grad_seg * attn_out, axis=-1)
        value_part = jnp.einsum('hqk,qhd->khd', probs_low, grad_seg)
        prob_grad = jnp.einsum('qhd,khd->hqk', grad_seg, value_band)
        score_grad = probs_full * (prob_grad - jnp.transpose(out_dot)[:, :, None])
        score_low = lax.optimization_barrier(score_grad.astype(jnp.bfloat16)).astype(jnp.float32)
        query_part = score_scale * jnp.einsum('hqk,khd->qhd', score_low, key_band)
        key_part = score_scale * jnp.einsum('hqk,qhd->khd', score_low, query_seg)
        key_acc = lax.dynamic_update_slice_in_dim(
            key_acc, lax.dynamic_slice_in_dim(key_acc, start, band, 0) + key_part, start, 0)
        value_acc = lax.dynamic_update_slice_in_dim(
            value_acc, lax.dynamic_slice_in_dim(value_acc, start, band, 0) + value_part, start, 0)
        pattern = pattern + score_grad
        return (key_acc, value_acc, pattern), query_part.astype(jnp.bfloat16)

    initial = (jnp.zeros((TOKENS + reach, HEADS, HDIM), jnp.float32),
               jnp.zeros((TOKENS + reach, HEADS, HDIM), jnp.float32),
               jnp.zeros((HEADS, SEG, band), jnp.float32))
    (key_acc, value_acc, pattern), query_parts = lax.scan(
        one_segment, initial, jnp.arange(TOKENS // SEG, dtype=jnp.int32))
    query_grad = query_parts.reshape(TOKENS, D)
    key_grad = key_acc[reach:].reshape(TOKENS, D).astype(jnp.bfloat16)
    value_grad = value_acc[reach:].reshape(TOKENS, D).astype(jnp.bfloat16)
    one_hot = (buckets[:, :, None] == jnp.arange(2 * MAXREL + 1, dtype=jnp.int32)[None, None, :]).astype(jnp.float32)
    table_grad = jnp.einsum('hqk,qkr->hr', pattern, one_hot, precision=lax.Precision.HIGHEST)
    query_weight_grad = jnp.dot(inputs.T, query_grad, preferred_element_type=jnp.float32)
    key_weight_grad = jnp.dot(inputs.T, key_grad, preferred_element_type=jnp.float32)
    value_weight_grad = jnp.dot(inputs.T, value_grad, preferred_element_type=jnp.float32)
    return (query_grad, key_grad, value_grad, query_weight_grad, key_weight_grad, value_weight_grad, table_grad)
```

```python
import functools

import jax
import jax.numpy as jnp
from jax import lax
from jax.experimental import pallas as pl
from jax.experimental.pallas import tpu as pltpu
from jax.sharding import PartitionSpec as P

HDIM = 128
SEG = 64
PREV = 4
MAXREL = 128
REACH = PREV * SEG
TILE = 2 * SEG
BAND = REACH + TILE
WRAP = 4 * MAXREL
GROUPS = 2


def from_behind(block, axis, distance):
    devices = range(lax.axis_size(axis))
    route = [(i - distance, i) for i in devices if i - distance in devices]
    return lax.ppermute(block, axis, route)


def project(inputs, weight):
    return jnp.dot(inputs, weight, preferred_element_type=jnp.float32).astype(jnp.bfloat16)


def contract(a, b, dims):
    return lax.dot_general(a, b, (dims, ((), ())), preferred_element_type=jnp.float32)


def attention_kernel(
    first_ref, bias_ref, q_ref, k_ref, v_ref, g_ref, hk_ref, hv_ref,
    dq_ref, dk_ref, dv_ref, hdk_ref, hdv_ref, tk_ref, tv_ref, diag_ref,
    kx, vx, dk_acc, dv_acc, band_acc,
):
    rows = q_ref.shape[0]
    scale = HDIM ** (-0.5)
    kx[:REACH] = hk_ref[...]
    kx[REACH:] = k_ref[...]
    vx[:REACH] = hv_ref[...]
    vx[REACH:] = v_ref[...]
    dk_acc[...] = jnp.zeros_like(dk_acc)
    dv_acc[...] = jnp.zeros_like(dv_acc)
    band_acc[...] = jnp.zeros_like(band_acc)
    row = lax.broadcasted_iota(jnp.int32, (TILE, BAND), 0)
    col = lax.broadcasted_iota(jnp.int32, (TILE, BAND), 1)
    start = row // SEG * SEG
    seen = (col >= start) & (col < start + REACH + SEG)
    wide = jnp.broadcast_to(bias_ref[0], (TILE, WRAP))
    bias = pltpu.roll(wide, 0, 1, stride=1, stride_axis=0)[:, :BAND]
    bias = jnp.where(seen, bias, -jnp.inf)
    is_first = first_ref[0] == 0
    for blk in range(rows // TILE):
        lo = blk * TILE
        q = q_ref[lo : lo + TILE]
        g = g_ref[lo : lo + TILE]
        k = kx[lo : lo + BAND]
        v = vx[lo : lo + BAND]
        s = contract(q, k, ((1,), (1,))) * scale + bias
        if lo < REACH:
            s = jnp.where(is_first & (col < REACH - lo), -jnp.inf, s)
        m = jnp.max(s, axis=1, keepdims=True)
        e = jnp.exp(s - m)
        p = e * (1.0 / jnp.sum(e, axis=1, keepdims=True))
        p_low = p.astype(jnp.bfloat16)
        out = contract(p_low, v, ((1,), (0,))).astype(jnp.bfloat16)
        out_dot = jnp.sum(g.astype(jnp.float32) * out.astype(jnp.float32), axis=1, keepdims=True)
        dp = contract(g, v, ((1,), (1,)))
        ds = p * (dp - out_dot)
        ds_low = ds.astype(jnp.bfloat16)
        band_acc[:, :BAND] += ds
        dq_ref[lo : lo + TILE] = (contract(ds_low, k, ((1,), (0,))) * scale).astype(jnp.bfloat16)
        dk_acc[lo : lo + BAND] += contract(ds_low, q, ((0,), (0,)))
        dv_acc[lo : lo + BAND] += contract(p_low, g, ((0,), (0,)))
    dk_ref[...] = (dk_acc[REACH:] * scale).astype(jnp.bfloat16)
    dv_ref[...] = dv_acc[REACH:].astype(jnp.bfloat16)
    hdk_ref[...] = (dk_acc[:REACH] * scale).astype(jnp.bfloat16)
    hdv_ref[...] = dv_acc[:REACH].astype(jnp.bfloat16)
    tk_ref[...] = dk_acc[rows:] * scale
    tv_ref[...] = dv_acc[rows:]
    total = band_acc[...]
    half = TILE // 2
    while half >= 1:
        total = total[:half] + pltpu.roll(total[half:], WRAP - half, 1)
        half //= 2
    diag_ref[0] = total


def attention(first, bias_rows, query, keys, values, upstream, halo_k, halo_v, head0, heads):
    rows = query.shape[0]
    whole = pl.BlockSpec((rows, HDIM), lambda h: (0, h))
    shifted = pl.BlockSpec((rows, HDIM), lambda h: (0, head0 + h))
    edge = pl.BlockSpec((REACH, HDIM), lambda h: (0, h))
    line = pl.BlockSpec((1, 1, WRAP), lambda h: (head0 + h, 0, 0))
    width = heads * HDIM
    sds = jax.ShapeDtypeStruct
    flops = 12 * heads * rows * BAND * HDIM
    return pl.pallas_call(
        attention_kernel,
        grid=(heads,),
        in_specs=[pl.BlockSpec(memory_space=pltpu.SMEM), line, shifted, shifted, shifted, shifted,
                  pl.BlockSpec((REACH, HDIM), lambda h: (0, h)), pl.BlockSpec((REACH, HDIM), lambda h: (0, h))],
        out_specs=[whole, whole, whole, edge, edge, edge, edge,
                   pl.BlockSpec((1, 1, WRAP), lambda h: (h, 0, 0))],
        out_shape=[
            sds((rows, width), jnp.bfloat16), sds((rows, width), jnp.bfloat16), sds((rows, width), jnp.bfloat16),
            sds((REACH, width), jnp.bfloat16), sds((REACH, width), jnp.bfloat16),
            sds((REACH, width), jnp.float32), sds((REACH, width), jnp.float32),
            sds((heads, 1, WRAP), jnp.float32),
        ],
        scratch_shapes=[
            pltpu.VMEM((rows + REACH, HDIM), jnp.bfloat16), pltpu.VMEM((rows + REACH, HDIM), jnp.bfloat16),
            pltpu.VMEM((rows + REACH, HDIM), jnp.float32), pltpu.VMEM((rows + REACH, HDIM), jnp.float32),
            pltpu.VMEM((TILE, WRAP), jnp.float32),
        ],
        cost_estimate=pl.CostEstimate(flops=flops * 2, bytes_accessed=heads * rows * HDIM * 20, transcendentals=heads * rows * BAND),
    )(first, bias_rows, query, keys, values, upstream, halo_k, halo_v)


def local(inputs, w_query, w_key, w_value, rel_table, out_grad):
    rows = inputs.shape[0]
    head_count = w_query.shape[1] // HDIM
    first = lax.axis_index("sp").reshape(1)
    far = rel_table[:, 2 * MAXREL :]
    pad = jnp.broadcast_to(far, (head_count, MAXREL))
    bias_rows = jnp.concatenate([pad, rel_table[:, :0:-1], pad], axis=1)[:, None, :]
    keys = project(inputs, w_key)
    values = project(inputs, w_value)
    halo = from_behind(jnp.concatenate([keys[rows - REACH :], values[rows - REACH :]], axis=1), "sp", 1)
    query = project(inputs, w_query)
    width = head_count * HDIM
    heads = head_count // GROUPS
    span = heads * HDIM
    grads, sums, diags = [], [], []
    for group in range(GROUPS):
        at = group * span
        dq, dk, dv, hdk, hdv, tk, tv, diag = attention(
            first, bias_rows, query, keys, values, out_grad,
            halo[:, at : at + span], halo[:, width + at : width + at + span], group * heads, heads)
        back = from_behind(jnp.concatenate([hdk, hdv], axis=1), "sp", -1).astype(jnp.float32)
        dk = lax.dynamic_update_slice(dk, (tk + back[:, :span]).astype(jnp.bfloat16), (rows - REACH, 0))
        dv = lax.dynamic_update_slice(dv, (tv + back[:, span:]).astype(jnp.bfloat16), (rows - REACH, 0))
        part = jnp.einsum("td,tc->dc", inputs, jnp.concatenate([dq, dk, dv], axis=1),
                          preferred_element_type=jnp.float32).astype(jnp.bfloat16)
        sums.append(lax.psum_scatter(part, "sp", scatter_dimension=0, tiled=True))
        grads.append((dq, dk, dv))
        diags.append(diag)
    query_grad, key_grad, value_grad = [jnp.concatenate(parts, axis=1) for parts in zip(*grads)]
    wq, wk, wv = [
        jnp.concatenate([s[:, i * span : (i + 1) * span] for s in sums], axis=1).astype(jnp.float32)
        for i in range(3)
    ]
    diag = lax.psum(jnp.concatenate(diags, axis=0)[:, 0, :], "sp")
    top = jnp.sum(diag[:, : MAXREL + 1], axis=1, keepdims=True) + jnp.sum(diag[:, 3 * MAXREL :], axis=1, keepdims=True)
    table_grad = jnp.concatenate(
        [jnp.zeros((head_count, 1), jnp.float32), diag[:, MAXREL + 1 : 3 * MAXREL][:, ::-1], top], axis=1)
    return query_grad, key_grad, value_grad, wq, wk, wv, table_grad


def solution(mesh):
    placed = (
        P("sp", None),
        P(None, "tp"),
        P(None, "tp"),
        P(None, "tp"),
        P("tp", None),
        P("sp", "tp"),
    )
    return jax.shard_map(
        local,
        mesh=mesh,
        in_specs=placed,
        out_specs=(
            P("sp", "tp"),
            P("sp", "tp"),
            P("sp", "tp"),
            P("sp", "tp"),
            P("sp", "tp"),
            P("sp", "tp"),
            P("tp", None),
        ),
        check_vma=False,
    )
```

```python
import functools

import jax
import jax.numpy as jnp
from jax import lax
from jax.experimental import pallas as pl
from jax.experimental.pallas import tpu as pltpu
from jax.sharding import PartitionSpec as P

HDIM = 128
SEG = 64
PREV = 4
MAXREL = 128
REACH = PREV * SEG
TILE = 2 * SEG
BAND = REACH + TILE
WRAP = 4 * MAXREL
GROUPS = 2


def from_behind(block, axis, distance):
    devices = range(lax.axis_size(axis))
    route = [(i - distance, i) for i in devices if i - distance in devices]
    return lax.ppermute(block, axis, route)


def project(inputs, weight):
    return jnp.dot(inputs, weight, preferred_element_type=jnp.float32).astype(jnp.bfloat16)


def contract(a, b, dims):
    return lax.dot_general(a, b, (dims, ((), ())), preferred_element_type=jnp.float32)


def attention_kernel(
    first_ref, bias_ref, q_ref, k_ref, v_ref, g_ref, hk_ref, hv_ref,
    dq_ref, dk_ref, dv_ref, hdk_ref, hdv_ref, tk_ref, tv_ref, diag_ref,
    kx, vx, dk_acc, dv_acc, band_acc,
):
    rows = q_ref.shape[0]
    scale = HDIM ** (-0.5)
    kx[:REACH] = hk_ref[...]
    kx[REACH:] = k_ref[...]
    vx[:REACH] = hv_ref[...]
    vx[REACH:] = v_ref[...]
    dk_acc[...] = jnp.zeros_like(dk_acc)
    dv_acc[...] = jnp.zeros_like(dv_acc)
    band_acc[...] = jnp.zeros_like(band_acc)
    row = lax.broadcasted_iota(jnp.int32, (TILE, BAND), 0)
    col = lax.broadcasted_iota(jnp.int32, (TILE, BAND), 1)
    start = row // SEG * SEG
    seen = (col >= start) & (col < start + REACH + SEG)
    wide = jnp.broadcast_to(bias_ref[0], (TILE, WRAP))
    bias = pltpu.roll(wide, 0, 1, stride=1, stride_axis=0)[:, :BAND]
    bias = jnp.where(seen, bias, -jnp.inf)
    is_first = first_ref[0] == 0
    for blk in range(rows // TILE):
        lo = blk * TILE
        q = q_ref[lo : lo + TILE]
        g = g_ref[lo : lo + TILE]
        k = kx[lo : lo + BAND]
        v = vx[lo : lo + BAND]
        s = contract(q, k, ((1,), (1,))) * scale + bias
        if lo < REACH:
            s = jnp.where(is_first & (col < REACH - lo), -jnp.inf, s)
        m = jnp.max(s, axis=1, keepdims=True)
        e = jnp.exp(s - m)
        p = e * (1.0 / jnp.sum(e, axis=1, keepdims=True))
        p_low = p.astype(jnp.bfloat16)
        out = contract(p_low, v, ((1,), (0,))).astype(jnp.bfloat16)
        out_dot = jnp.sum(g.astype(jnp.float32) * out.astype(jnp.float32), axis=1, keepdims=True)
        dp = contract(g, v, ((1,), (1,)))
        ds = p * (dp - out_dot)
        ds_low = ds.astype(jnp.bfloat16)
        band_acc[:, :BAND] += ds
        dq_ref[lo : lo + TILE] = (contract(ds_low, k, ((1,), (0,))) * scale).astype(jnp.bfloat16)
        dk_acc[lo : lo + BAND] += contract(ds_low, q, ((0,), (0,)))
        dv_acc[lo : lo + BAND] += contract(p_low, g, ((0,), (0,)))
    dk_ref[...] = (dk_acc[REACH:] * scale).astype(jnp.bfloat16)
    dv_ref[...] = dv_acc[REACH:].astype(jnp.bfloat16)
    hdk_ref[...] = (dk_acc[:REACH] * scale).astype(jnp.bfloat16)
    hdv_ref[...] = dv_acc[:REACH].astype(jnp.bfloat16)
    tk_ref[...] = dk_acc[rows:] * scale
    tv_ref[...] = dv_acc[rows:]
    total = band_acc[...]
    half = TILE // 2
    while half >= 1:
        total = total[:half] + pltpu.roll(total[half:], WRAP - half, 1)
        half //= 2
    diag_ref[0] = total


def attention(first, bias_rows, query, keys, values, upstream, halo_k, halo_v, head0, heads):
    rows = query.shape[0]
    whole = pl.BlockSpec((rows, HDIM), lambda h: (0, h))
    shifted = pl.BlockSpec((rows, HDIM), lambda h: (0, head0 + h))
    edge = pl.BlockSpec((REACH, HDIM), lambda h: (0, h))
    line = pl.BlockSpec((1, 1, WRAP), lambda h: (head0 + h, 0, 0))
    width = heads * HDIM
    sds = jax.ShapeDtypeStruct
    flops = 12 * heads * rows * BAND * HDIM
    return pl.pallas_call(
        attention_kernel,
        grid=(heads,),
        in_specs=[pl.BlockSpec(memory_space=pltpu.SMEM), line, shifted, shifted, shifted, shifted,
                  pl.BlockSpec((REACH, HDIM), lambda h: (0, h)), pl.BlockSpec((REACH, HDIM), lambda h: (0, h))],
        out_specs=[whole, whole, whole, edge, edge, edge, edge,
                   pl.BlockSpec((1, 1, WRAP), lambda h: (h, 0, 0))],
        out_shape=[
            sds((rows, width), jnp.bfloat16), sds((rows, width), jnp.bfloat16), sds((rows, width), jnp.bfloat16),
            sds((REACH, width), jnp.bfloat16), sds((REACH, width), jnp.bfloat16),
            sds((REACH, width), jnp.float32), sds((REACH, width), jnp.float32),
            sds((heads, 1, WRAP), jnp.float32),
        ],
        scratch_shapes=[
            pltpu.VMEM((rows + REACH, HDIM), jnp.bfloat16), pltpu.VMEM((rows + REACH, HDIM), jnp.bfloat16),
            pltpu.VMEM((rows + REACH, HDIM), jnp.float32), pltpu.VMEM((rows + REACH, HDIM), jnp.float32),
            pltpu.VMEM((TILE, WRAP), jnp.float32),
        ],
        cost_estimate=pl.CostEstimate(flops=flops * 2, bytes_accessed=heads * rows * HDIM * 20, transcendentals=heads * rows * BAND),
    )(first, bias_rows, query, keys, values, upstream, halo_k, halo_v)


def swap(block, bit):
    size = lax.axis_size("sp")
    return lax.ppermute(block, "sp", [(i, i ^ (1 << bit)) for i in range(size)])


def scatter_sum(sides, grads, order):
    sent_lhs, kept_lhs, kept = sides[order[0]]
    sent = jnp.einsum("td,tc->dc", sent_lhs, grads, preferred_element_type=jnp.float32).astype(jnp.bfloat16)
    came = swap(sent, order[0])
    total = jnp.einsum("td,tc->dc", kept_lhs, grads, preferred_element_type=jnp.float32)
    total = total + came.astype(jnp.float32)
    depth = total.shape[0] // len(kept)
    for bit in order[1:]:
        out = [i for i, r in enumerate(kept) if r >> bit & 1]
        stay = [i for i, r in enumerate(kept) if not r >> bit & 1]
        pick = lambda which: jnp.concatenate([total[i * depth : (i + 1) * depth] for i in which], axis=0)
        came = swap(pick(out).astype(jnp.bfloat16), bit)
        total = pick(stay) + came.astype(jnp.float32)
        kept = [kept[i] for i in stay]
    return total


def local(inputs, w_query, w_key, w_value, rel_table, out_grad):
    rows, model = inputs.shape
    head_count = w_query.shape[1] // HDIM
    size = lax.axis_size("sp")
    bits = size.bit_length() - 1
    me = lax.axis_index("sp")
    first = me.reshape(1)
    far = rel_table[:, 2 * MAXREL :]
    pad = jnp.broadcast_to(far, (head_count, MAXREL))
    bias_rows = jnp.concatenate([pad, rel_table[:, :0:-1], pad], axis=1)[:, None, :]
    keys = project(inputs, w_key)
    values = project(inputs, w_value)
    halo = from_behind(jnp.concatenate([keys[rows - REACH :], values[rows - REACH :]], axis=1), "sp", 1)
    query = project(inputs, w_query)
    width = head_count * HDIM
    heads = head_count // GROUPS
    span = heads * HDIM
    depth = model // size
    block = lambda r: lax.dynamic_slice(inputs, (0, (me ^ r) * depth), (rows, depth))
    sides = {}
    for lead in {order[0] for order in chunk_orders(bits)}:
        out = [r for r in range(size) if r >> lead & 1]
        stay = [r for r in range(size) if not r >> lead & 1]
        sides[lead] = (jnp.concatenate([block(r) for r in out], axis=1),
                       jnp.concatenate([block(r) for r in stay], axis=1), stay)
    grads, sums, diags = [], [], []
    for group in range(GROUPS):
        at = group * span
        dq, dk, dv, hdk, hdv, tk, tv, diag = attention(
            first, bias_rows, query, keys, values, out_grad,
            halo[:, at : at + span], halo[:, width + at : width + at + span], group * heads, heads)
        back = from_behind(jnp.concatenate([hdk, hdv], axis=1), "sp", -1).astype(jnp.float32)
        dk = lax.dynamic_update_slice(dk, (tk + back[:, :span]).astype(jnp.bfloat16), (rows - REACH, 0))
        dv = lax.dynamic_update_slice(dv, (tv + back[:, span:]).astype(jnp.bfloat16), (rows - REACH, 0))
        orders = chunk_orders(bits)[3 * group : 3 * group + 3]
        sums.append([scatter_sum(sides, grad, order) for grad, order in zip((dq, dk, dv), orders)])
        grads.append((dq, dk, dv))
        diags.append(diag)
    query_grad, key_grad, value_grad = [jnp.concatenate(parts, axis=1) for parts in zip(*grads)]
    wq, wk, wv = [jnp.concatenate(parts, axis=1) for parts in zip(*sums)]
    diag = jnp.concatenate(diags, axis=0)[:, 0, :]
    for bit in range(bits):
        diag = diag + swap(diag, bit)
    top = jnp.sum(diag[:, : MAXREL + 1], axis=1, keepdims=True) + jnp.sum(diag[:, 3 * MAXREL :], axis=1, keepdims=True)
    table_grad = jnp.concatenate(
        [jnp.zeros((head_count, 1), jnp.float32), diag[:, MAXREL + 1 : 3 * MAXREL][:, ::-1], top], axis=1)
    return query_grad, key_grad, value_grad, wq, wk, wv, table_grad


def chunk_orders(bits):
    plain = list(range(bits))
    return [plain] * (3 * GROUPS)


def solution(mesh):
    placed = (
        P("sp", None),
        P(None, "tp"),
        P(None, "tp"),
        P(None, "tp"),
        P("tp", None),
        P("sp", "tp"),
    )
    return jax.shard_map(
        local,
        mesh=mesh,
        in_specs=placed,
        out_specs=(
            P("sp", "tp"),
            P("sp", "tp"),
            P("sp", "tp"),
            P("sp", "tp"),
            P("sp", "tp"),
            P("sp", "tp"),
            P("tp", None),
        ),
        check_vma=False,
    )
```

```python
import jax
import jax.numpy as jnp
from jax import lax
from jax.experimental import pallas as pl
from jax.experimental.pallas import tpu as pltpu
from jax.sharding import PartitionSpec as P


HDIM = 128
SEG = 64
PREV = 4
MAXREL = 128
REACH = PREV * SEG
TILE = 2 * SEG
BAND = REACH + TILE
WRAP = 4 * MAXREL
GROUPS = 2


def from_behind(block, axis, distance):
    devices = range(lax.axis_size(axis))
    route = [(i - distance, i) for i in devices if i - distance in devices]
    return lax.ppermute(block, axis, route)


def project(inputs, weight):
    return jnp.dot(inputs, weight, preferred_element_type=jnp.float32).astype(jnp.bfloat16)


def contract(a, b, dims):
    return lax.dot_general(a, b, (dims, ((), ())), preferred_element_type=jnp.float32)


def attention_kernel(
    first_ref, bias_ref, q_ref, k_ref, v_ref, g_ref, hk_ref, hv_ref,
    dq_ref, dk_ref, dv_ref, hdk_ref, hdv_ref, tk_ref, tv_ref, diag_ref,
    kx, vx, dk_acc, dv_acc, band_acc,
):
    rows = q_ref.shape[0]
    scale = HDIM ** (-0.5)
    kx[:REACH] = hk_ref[...]
    kx[REACH:] = k_ref[...]
    vx[:REACH] = hv_ref[...]
    vx[REACH:] = v_ref[...]
    dk_acc[...] = jnp.zeros_like(dk_acc)
    dv_acc[...] = jnp.zeros_like(dv_acc)
    band_acc[...] = jnp.zeros_like(band_acc)
    row = lax.broadcasted_iota(jnp.int32, (TILE, BAND), 0)
    col = lax.broadcasted_iota(jnp.int32, (TILE, BAND), 1)
    start = row // SEG * SEG
    seen = (col >= start) & (col < start + REACH + SEG)
    wide = jnp.broadcast_to(bias_ref[0], (TILE, WRAP))
    bias = pltpu.roll(wide, 0, 1, stride=1, stride_axis=0)[:, :BAND]
    bias = jnp.where(seen, bias, -jnp.inf)
    is_first = first_ref[0] == 0
    for blk in range(rows // TILE):
        lo = blk * TILE
        q = q_ref[lo : lo + TILE]
        g = g_ref[lo : lo + TILE]
        k = kx[lo : lo + BAND]
        v = vx[lo : lo + BAND]
        s = contract(q, k, ((1,), (1,))) * scale + bias
        if lo < REACH:
            s = jnp.where(is_first & (col < REACH - lo), -jnp.inf, s)
        m = jnp.max(s, axis=1, keepdims=True)
        e = jnp.exp(s - m)
        p = e * (1.0 / jnp.sum(e, axis=1, keepdims=True))
        p_low = p.astype(jnp.bfloat16)
        out = contract(p_low, v, ((1,), (0,))).astype(jnp.bfloat16)
        out_dot = jnp.sum(g.astype(jnp.float32) * out.astype(jnp.float32), axis=1, keepdims=True)
        dp = contract(g, v, ((1,), (1,)))
        ds = p * (dp - out_dot)
        ds_low = ds.astype(jnp.bfloat16)
        band_acc[:, :BAND] += ds
        dq_ref[lo : lo + TILE] = (contract(ds_low, k, ((1,), (0,))) * scale).astype(jnp.bfloat16)
        dk_acc[lo : lo + BAND] += contract(ds_low, q, ((0,), (0,)))
        dv_acc[lo : lo + BAND] += contract(p_low, g, ((0,), (0,)))
    dk_ref[...] = (dk_acc[REACH:] * scale).astype(jnp.bfloat16)
    dv_ref[...] = dv_acc[REACH:].astype(jnp.bfloat16)
    hdk_ref[...] = (dk_acc[:REACH] * scale).astype(jnp.bfloat16)
    hdv_ref[...] = dv_acc[:REACH].astype(jnp.bfloat16)
    tk_ref[...] = dk_acc[rows:] * scale
    tv_ref[...] = dv_acc[rows:]
    total = band_acc[...]
    half = TILE // 2
    while half >= 1:
        total = total[:half] + pltpu.roll(total[half:], WRAP - half, 1)
        half //= 2
    diag_ref[0] = total


def attention(first, bias_rows, query, keys, values, upstream, halo_k, halo_v, head0, heads):
    rows = query.shape[0]
    whole = pl.BlockSpec((rows, HDIM), lambda h: (0, h))
    shifted = pl.BlockSpec((rows, HDIM), lambda h: (0, head0 + h))
    edge = pl.BlockSpec((REACH, HDIM), lambda h: (0, h))
    line = pl.BlockSpec((1, 1, WRAP), lambda h: (head0 + h, 0, 0))
    width = heads * HDIM
    sds = jax.ShapeDtypeStruct
    flops = 12 * heads * rows * BAND * HDIM
    return pl.pallas_call(
        attention_kernel,
        grid=(heads,),
        in_specs=[pl.BlockSpec(memory_space=pltpu.SMEM), line, shifted, shifted, shifted, shifted,
                  pl.BlockSpec((REACH, HDIM), lambda h: (0, h)), pl.BlockSpec((REACH, HDIM), lambda h: (0, h))],
        out_specs=[whole, whole, whole, edge, edge, edge, edge,
                   pl.BlockSpec((1, 1, WRAP), lambda h: (h, 0, 0))],
        out_shape=[
            sds((rows, width), jnp.bfloat16), sds((rows, width), jnp.bfloat16), sds((rows, width), jnp.bfloat16),
            sds((REACH, width), jnp.bfloat16), sds((REACH, width), jnp.bfloat16),
            sds((REACH, width), jnp.float32), sds((REACH, width), jnp.float32),
            sds((heads, 1, WRAP), jnp.float32),
        ],
        scratch_shapes=[
            pltpu.VMEM((rows + REACH, HDIM), jnp.bfloat16), pltpu.VMEM((rows + REACH, HDIM), jnp.bfloat16),
            pltpu.VMEM((rows + REACH, HDIM), jnp.float32), pltpu.VMEM((rows + REACH, HDIM), jnp.float32),
            pltpu.VMEM((TILE, WRAP), jnp.float32),
        ],
        cost_estimate=pl.CostEstimate(flops=flops * 2, bytes_accessed=heads * rows * HDIM * 20, transcendentals=heads * rows * BAND),
    )(first, bias_rows, query, keys, values, upstream, halo_k, halo_v)


def swap(block, bit):
    size = lax.axis_size("sp")
    return lax.ppermute(block, "sp", [(i, i ^ (1 << bit)) for i in range(size)])


def side(pieces, lead, want):
    low = len(pieces)
    return [pieces[r] for r in range(low) if (r >> lead & 1) == want]


def product(lhs, grads):
    parts = [jnp.einsum("td,tc->dc", piece, grads, preferred_element_type=jnp.float32) for piece in lhs]
    return parts


def leading(pieces, grads, order):
    return jnp.concatenate([p.astype(jnp.bfloat16) for p in product(side(pieces, order[0], 1), grads)], axis=0)


def remainder(pieces, grads, order, came):
    total = jnp.concatenate(product(side(pieces, order[0], 0), grads), axis=0)
    return total + came.astype(jnp.float32)


def split(total, kept, bit):
    depth = total.shape[0] // len(kept)
    out = [i for i, r in enumerate(kept) if r >> bit & 1]
    stay = [i for i, r in enumerate(kept) if not r >> bit & 1]
    pick = lambda which: jnp.concatenate([total[i * depth : (i + 1) * depth] for i in which], axis=0)
    return pick(out).astype(jnp.bfloat16), pick(stay), [kept[i] for i in stay]


def local(inputs, w_query, w_key, w_value, rel_table, out_grad):
    rows, model = inputs.shape
    head_count = w_query.shape[1] // HDIM
    size = lax.axis_size("sp")
    bits = size.bit_length() - 1
    me = lax.axis_index("sp")
    first = me.reshape(1)
    far = rel_table[:, 2 * MAXREL :]
    pad = jnp.broadcast_to(far, (head_count, MAXREL))
    bias_rows = jnp.concatenate([pad, rel_table[:, :0:-1], pad], axis=1)[:, None, :]
    keys = project(inputs, w_key)
    values = project(inputs, w_value)
    halo = from_behind(jnp.concatenate([keys[rows - REACH :], values[rows - REACH :]], axis=1), "sp", 1)
    query = project(inputs, w_query)
    width = head_count * HDIM
    heads = head_count // GROUPS
    span = heads * HDIM
    depth = model // size
    block = lambda r: lax.dynamic_slice(inputs, (0, (me ^ r) * depth), (rows, depth))
    low = min(size, 4)
    members = [[r for r in range(size) if r % low == p] for p in range(low)]
    pieces = [jnp.concatenate([block(r) for r in rs], axis=1) for rs in members]
    orders, ready = chunk_plan(bits)
    grads, chunks, flying, diags = [], [], [], []
    for group in range(GROUPS):
        at = group * span
        dq, dk, dv, hdk, hdv, tk, tv, diag = attention(
            first, bias_rows, query, keys, values, out_grad,
            halo[:, at : at + span], halo[:, width + at : width + at + span], group * heads, heads)
        back = jnp.concatenate([hdk, hdv], axis=1)
        sent = leading(pieces, dq, orders[3 * group])
        if group + 1 < GROUPS:
            back, sent, query = lax.optimization_barrier((back, sent, query))
        back = from_behind(back, "sp", -1).astype(jnp.float32)
        flying.append(swap(sent, orders[3 * group][0]))
        dk = lax.dynamic_update_slice(dk, (tk + back[:, :span]).astype(jnp.bfloat16), (rows - REACH, 0))
        dv = lax.dynamic_update_slice(dv, (tv + back[:, span:]).astype(jnp.bfloat16), (rows - REACH, 0))
        for i, grad in ((1, dk), (2, dv)):
            order = orders[3 * group + i]
            flying.append(swap(leading(pieces, grad, order), order[0]))
        grads.append((dq, dk, dv))
        chunks.extend((dq, dk, dv))
        diags.append(diag)
    count = len(chunks)
    kept = [[r for p in range(low) if not p >> order[0] & 1 for r in members[p]] for order in orders]
    held = [None] * count
    steps = sorted(((c, s) for c in range(count) for s in range(bits)), key=lambda cs: (ready[cs[0]] + 0.95 * cs[1], cs))
    last = None
    for c, stage in steps:
        came = flying[c]
        if last is not None:
            came, held[last] = lax.optimization_barrier((came, held[last]))
        if stage == 0:
            held[c] = remainder(pieces, chunks[c], orders[c], came)
        else:
            held[c] = held[c] + came.astype(jnp.float32)
        if stage + 1 < bits:
            bit = orders[c][stage + 1]
            out, held[c], kept[c] = split(held[c], kept[c], bit)
            flying[c] = swap(out, bit)
        last = c
    sums = [held[3 * group : 3 * group + 3] for group in range(GROUPS)]
    query_grad, key_grad, value_grad = [jnp.concatenate(parts, axis=1) for parts in zip(*grads)]
    wq, wk, wv = [jnp.concatenate(parts, axis=1) for parts in zip(*sums)]
    diag = jnp.concatenate(diags, axis=0)[:, 0, :]
    diag, _ = lax.optimization_barrier((diag, held[0]))
    for bit in range(bits):
        diag = diag + swap(diag, bit)
    top = jnp.sum(diag[:, : MAXREL + 1], axis=1, keepdims=True) + jnp.sum(diag[:, 3 * MAXREL :], axis=1, keepdims=True)
    table_grad = jnp.concatenate(
        [jnp.zeros((head_count, 1), jnp.float32), diag[:, MAXREL + 1 : 3 * MAXREL][:, ::-1], top], axis=1)
    return query_grad, key_grad, value_grad, wq, wk, wv, table_grad


def chunk_plan(bits):
    plain = list(range(bits))
    turned = [1, 0] + plain[2:] if bits > 1 else plain
    count = 3 * GROUPS
    orders = [plain] * (count - 2) + [turned] * 2
    ready = [1.0 + i for i in range(count - 2)] + [count - 2.1, count - 1.9]
    return orders, ready


def solution(mesh):
    placed = (
        P("sp", None),
        P(None, "tp"),
        P(None, "tp"),
        P(None, "tp"),
        P("tp", None),
        P("sp", "tp"),
    )
    return jax.shard_map(
        local,
        mesh=mesh,
        in_specs=placed,
        out_specs=(
            P("sp", "tp"),
            P("sp", "tp"),
            P("sp", "tp"),
            P("sp", "tp"),
            P("sp", "tp"),
            P("sp", "tp"),
            P("tp", None),
        ),
        check_vma=False,
    )
```

```python
import jax
import jax.numpy as jnp
from jax import lax
from jax.experimental import pallas as pl
from jax.experimental.pallas import tpu as pltpu
from jax.sharding import PartitionSpec as P


HDIM = 128
SEG = 64
PREV = 4
MAXREL = 128
REACH = PREV * SEG
TILE = 2 * SEG
BAND = REACH + TILE
WRAP = 4 * MAXREL
GROUPS = 2


def from_behind(block, axis, distance):
    devices = range(lax.axis_size(axis))
    route = [(i - distance, i) for i in devices if i - distance in devices]
    return lax.ppermute(block, axis, route)


def project(inputs, weight):
    return jnp.dot(inputs, weight, preferred_element_type=jnp.float32).astype(jnp.bfloat16)


def contract(a, b, dims):
    return lax.dot_general(a, b, (dims, ((), ())), preferred_element_type=jnp.float32)


def attention_kernel(
    first_ref, bias_ref, q_ref, k_ref, v_ref, g_ref, hk_ref, hv_ref,
    dq_ref, dk_ref, dv_ref, hdk_ref, hdv_ref, tk_ref, tv_ref, diag_ref,
    kx, vx, dk_acc, dv_acc, band_acc,
):
    rows = q_ref.shape[0]
    scale = HDIM ** (-0.5)
    kx[:REACH] = hk_ref[...]
    kx[REACH:] = k_ref[...]
    vx[:REACH] = hv_ref[...]
    vx[REACH:] = v_ref[...]
    dk_acc[...] = jnp.zeros_like(dk_acc)
    dv_acc[...] = jnp.zeros_like(dv_acc)
    band_acc[...] = jnp.zeros_like(band_acc)
    row = lax.broadcasted_iota(jnp.int32, (TILE, BAND), 0)
    col = lax.broadcasted_iota(jnp.int32, (TILE, BAND), 1)
    start = row // SEG * SEG
    seen = (col >= start) & (col < start + REACH + SEG)
    wide = jnp.broadcast_to(bias_ref[0], (TILE, WRAP))
    bias = pltpu.roll(wide, 0, 1, stride=1, stride_axis=0)[:, :BAND]
    bias = jnp.where(seen, bias, -jnp.inf)
    is_first = first_ref[0] == 0
    for blk in range(rows // TILE):
        lo = blk * TILE
        q = q_ref[lo : lo + TILE]
        g = g_ref[lo : lo + TILE]
        k = kx[lo : lo + BAND]
        v = vx[lo : lo + BAND]
        s = contract(q, k, ((1,), (1,))) * scale + bias
        if lo < REACH:
            s = jnp.where(is_first & (col < REACH - lo), -jnp.inf, s)
        m = jnp.max(s, axis=1, keepdims=True)
        e = jnp.exp(s - m)
        p = e * (1.0 / jnp.sum(e, axis=1, keepdims=True))
        p_low = p.astype(jnp.bfloat16)
        out = contract(p_low, v, ((1,), (0,))).astype(jnp.bfloat16)
        out_dot = jnp.sum(g.astype(jnp.float32) * out.astype(jnp.float32), axis=1, keepdims=True)
        dp = contract(g, v, ((1,), (1,)))
        ds = p * (dp - out_dot)
        ds_low = ds.astype(jnp.bfloat16)
        band_acc[:, :BAND] += ds
        dq_ref[lo : lo + TILE] = (contract(ds_low, k, ((1,), (0,))) * scale).astype(jnp.bfloat16)
        dk_acc[lo : lo + BAND] += contract(ds_low, q, ((0,), (0,)))
        dv_acc[lo : lo + BAND] += contract(p_low, g, ((0,), (0,)))
    dk_ref[...] = (dk_acc[REACH:] * scale).astype(jnp.bfloat16)
    dv_ref[...] = dv_acc[REACH:].astype(jnp.bfloat16)
    hdk_ref[...] = (dk_acc[:REACH] * scale).astype(jnp.bfloat16)
    hdv_ref[...] = dv_acc[:REACH].astype(jnp.bfloat16)
    tk_ref[...] = dk_acc[rows:] * scale
    tv_ref[...] = dv_acc[rows:]
    total = band_acc[...]
    half = TILE // 2
    while half >= 1:
        total = total[:half] + pltpu.roll(total[half:], WRAP - half, 1)
        half //= 2
    diag_ref[0] = total


def attention(first, bias_rows, query, keys, values, upstream, halo_k, halo_v, head0, heads):
    rows = query.shape[0]
    whole = pl.BlockSpec((rows, HDIM), lambda h: (0, h))
    shifted = pl.BlockSpec((rows, HDIM), lambda h: (0, head0 + h))
    edge = pl.BlockSpec((REACH, HDIM), lambda h: (0, h))
    line = pl.BlockSpec((1, 1, WRAP), lambda h: (head0 + h, 0, 0))
    width = heads * HDIM
    sds = jax.ShapeDtypeStruct
    flops = 12 * heads * rows * BAND * HDIM
    return pl.pallas_call(
        attention_kernel,
        grid=(heads,),
        in_specs=[pl.BlockSpec(memory_space=pltpu.SMEM), line, shifted, shifted, shifted, shifted,
                  pl.BlockSpec((REACH, HDIM), lambda h: (0, h)), pl.BlockSpec((REACH, HDIM), lambda h: (0, h))],
        out_specs=[whole, whole, whole, edge, edge, edge, edge,
                   pl.BlockSpec((1, 1, WRAP), lambda h: (h, 0, 0))],
        out_shape=[
            sds((rows, width), jnp.bfloat16), sds((rows, width), jnp.bfloat16), sds((rows, width), jnp.bfloat16),
            sds((REACH, width), jnp.bfloat16), sds((REACH, width), jnp.bfloat16),
            sds((REACH, width), jnp.float32), sds((REACH, width), jnp.float32),
            sds((heads, 1, WRAP), jnp.float32),
        ],
        scratch_shapes=[
            pltpu.VMEM((rows + REACH, HDIM), jnp.bfloat16), pltpu.VMEM((rows + REACH, HDIM), jnp.bfloat16),
            pltpu.VMEM((rows + REACH, HDIM), jnp.float32), pltpu.VMEM((rows + REACH, HDIM), jnp.float32),
            pltpu.VMEM((TILE, WRAP), jnp.float32),
        ],
        cost_estimate=pl.CostEstimate(flops=flops * 2, bytes_accessed=heads * rows * HDIM * 20, transcendentals=heads * rows * BAND),
    )(first, bias_rows, query, keys, values, upstream, halo_k, halo_v)


def swap(block, bit):
    size = lax.axis_size("sp")
    return lax.ppermute(block, "sp", [(i, i ^ (1 << bit)) for i in range(size)])


def side(pieces, lead, want):
    low = len(pieces)
    return [pieces[r] for r in range(low) if (r >> lead & 1) == want]


def product(lhs, grads):
    parts = [jnp.einsum("td,tc->dc", piece, grads, preferred_element_type=jnp.float32) for piece in lhs]
    return parts


def leading(pieces, grads, order):
    return jnp.concatenate([p.astype(jnp.bfloat16) for p in product(side(pieces, order[0], 1), grads)], axis=0)


def remainder(pieces, grads, order, came):
    total = jnp.concatenate(product(side(pieces, order[0], 0), grads), axis=0)
    return total + came.astype(jnp.float32)


def split(total, kept, bit):
    depth = total.shape[0] // len(kept)
    out = [i for i, r in enumerate(kept) if r >> bit & 1]
    stay = [i for i, r in enumerate(kept) if not r >> bit & 1]
    pick = lambda which: jnp.concatenate([total[i * depth : (i + 1) * depth] for i in which], axis=0)
    return pick(out).astype(jnp.bfloat16), pick(stay), [kept[i] for i in stay]


def local(inputs, w_query, w_key, w_value, rel_table, out_grad):
    rows, model = inputs.shape
    head_count = w_query.shape[1] // HDIM
    size = lax.axis_size("sp")
    bits = size.bit_length() - 1
    me = lax.axis_index("sp")
    first = me.reshape(1)
    far = rel_table[:, 2 * MAXREL :]
    pad = jnp.broadcast_to(far, (head_count, MAXREL))
    bias_rows = jnp.concatenate([pad, rel_table[:, :0:-1], pad], axis=1)[:, None, :]
    keys = project(inputs, w_key)
    values = project(inputs, w_value)
    halo = from_behind(jnp.concatenate([keys[rows - REACH :], values[rows - REACH :]], axis=1), "sp", 1)
    query = project(inputs, w_query)
    width = head_count * HDIM
    heads = head_count // GROUPS
    span = heads * HDIM
    depth = model // size
    block = lambda r: lax.dynamic_slice(inputs, (0, (me ^ r) * depth), (rows, depth))
    low = min(size, 4)
    members = [[r for r in range(size) if r % low == p] for p in range(low)]
    pieces = [jnp.concatenate([block(r) for r in rs], axis=1) for rs in members]
    orders, ready = chunk_plan(bits)
    grads, chunks, flying, diags = [], [], [], []
    for group in range(GROUPS):
        at = group * span
        dq, dk, dv, hdk, hdv, tk, tv, diag = attention(
            first, bias_rows, query, keys, values, out_grad,
            halo[:, at : at + span], halo[:, width + at : width + at + span], group * heads, heads)
        back = jnp.concatenate([hdk, hdv], axis=1)
        sent = leading(pieces, dq, orders[3 * group])
        if group + 1 < GROUPS:
            back, sent, query = lax.optimization_barrier((back, sent, query))
        back = from_behind(back, "sp", -1).astype(jnp.float32)
        flying.append(swap(sent, orders[3 * group][0]))
        dk = lax.dynamic_update_slice(dk, (tk + back[:, :span]).astype(jnp.bfloat16), (rows - REACH, 0))
        dv = lax.dynamic_update_slice(dv, (tv + back[:, span:]).astype(jnp.bfloat16), (rows - REACH, 0))
        for i, grad in ((1, dk), (2, dv)):
            order = orders[3 * group + i]
            sent = leading(pieces, grad, order)
            flying.append(swap(sent, order[0]))
        grads.append((dq, dk, dv))
        chunks.extend((dq, dk, dv))
        diags.append(diag)
    count = len(chunks)
    kept = [[r for p in range(low) if not p >> order[0] & 1 for r in members[p]] for order in orders]
    held = [None] * count
    steps = sorted(((c, s) for c in range(count) for s in range(bits)), key=lambda cs: (ready[cs[0]] + 0.95 * cs[1], cs))
    last, done, hop = None, 0, 0
    diag = jnp.concatenate(diags, axis=0)[:, 0, :]
    table_came = swap(diag, 0)
    for c, stage in steps:
        came = flying[c]
        if last is not None:
            came, held[last] = lax.optimization_barrier((came, held[last]))
        if stage == 0:
            held[c] = remainder(pieces, chunks[c], orders[c], came)
        else:
            held[c] = held[c] + came.astype(jnp.float32)
        if stage + 1 < bits:
            bit = orders[c][stage + 1]
            out, held[c], kept[c] = split(held[c], kept[c], bit)
            flying[c] = swap(out, bit)
        last = c
        done += 1
        if hop < bits and done >= len(steps) * (hop + 1) // (bits + 1):
            came, held[c] = lax.optimization_barrier((table_came, held[c]))
            diag = diag + came
            hop += 1
            if hop < bits:
                table_came = swap(diag, hop)
    sums = [held[3 * group : 3 * group + 3] for group in range(GROUPS)]
    query_grad, key_grad, value_grad = [jnp.concatenate(parts, axis=1) for parts in zip(*grads)]
    wq, wk, wv = [jnp.concatenate(parts, axis=1) for parts in zip(*sums)]
    top = jnp.sum(diag[:, : MAXREL + 1], axis=1, keepdims=True) + jnp.sum(diag[:, 3 * MAXREL :], axis=1, keepdims=True)
    table_grad = jnp.concatenate(
        [jnp.zeros((head_count, 1), jnp.float32), diag[:, MAXREL + 1 : 3 * MAXREL][:, ::-1], top], axis=1)
    return query_grad, key_grad, value_grad, wq, wk, wv, table_grad


def chunk_plan(bits):
    plain = list(range(bits))
    turned = [1, 0] + plain[2:] if bits > 1 else plain
    count = 3 * GROUPS
    orders = [plain] * (count - 2) + [turned] * 2
    ready = [1.0, 3.0, 4.0, 2.0, 3.9, 4.1]
    return orders, ready


def solution(mesh):
    placed = (
        P("sp", None),
        P(None, "tp"),
        P(None, "tp"),
        P(None, "tp"),
        P("tp", None),
        P("sp", "tp"),
    )
    return jax.shard_map(
        local,
        mesh=mesh,
        in_specs=placed,
        out_specs=(
            P("sp", "tp"),
            P("sp", "tp"),
            P("sp", "tp"),
            P("sp", "tp"),
            P("sp", "tp"),
            P("sp", "tp"),
            P("tp", None),
        ),
        check_vma=False,
    )
```
